32 devices in a mesh: grp: 2 (over y), dp: 2 (over x), kv: 4 (over z), tp: 2 (over core).
Axes of the slice: x: 2, y: 2, z: 4, core: 2. Of those that a mesh axis runs over, the one named last changes fastest.
Arguments:
- residual_input: bfloat16 [128, 4096], P(('grp', 'dp', 'tp'), 'kv'), parts along dimension 0, may hold values from -6 to 6
- incoming_state: float32 [128, 16, 64, 128], P(('grp', 'kv'), ('dp', 'tp')), parts along dimension 0, may hold values from -4 to 4
- extra_log_decay: float32 [128, 1024], P(('grp', 'kv'), ('dp', 'tp')), parts along dimension 0, may hold values from -0.7 to 0
- leading_norm_gain: float32 [4096], P('kv'), may hold values from 0.1 to 1.9
- leading_gate_weight: bfloat16 [4096, 11264], P('kv', ('dp', 'tp')), may hold values from -0.09375 to 0.09375
- leading_up_weight: bfloat16 [4096, 11264], P('kv', ('dp', 'tp')), may hold values from -0.09375 to 0.09375
- leading_down_weight: bfloat16 [11264, 4096], P(('dp', 'tp'), 'kv'), may hold values from -0.0546875 to 0.0546875
- attention_norm_gain: float32 [4096], P('kv'), may hold values from 0.1 to 1.9
- query_projector: bfloat16 [4096, 1024], P('kv', ('dp', 'tp')), may hold values from -0.09375 to 0.09375
- key_projector: bfloat16 [4096, 1024], P('kv', ('dp', 'tp')), may hold values from -0.09375 to 0.09375
- value_projector: bfloat16 [4096, 2048], P('kv', ('dp', 'tp')), may hold values from -0.09375 to 0.09375
- output_gate_weight: bfloat16 [4096, 2048], P('kv', ('dp', 'tp')), may hold values from -0.09375 to 0.09375
- forget_weight: bfloat16 [4096, 1024], P('kv', ('dp', 'tp')), may hold values from -0.75 to 0.75
- head_norm_gain: float32 [128], replicated, may hold values from 0.1 to 1.9
- output_projector: bfloat16 [2048, 4096], P(('dp', 'tp'), 'kv'), may hold values from -0.125 to 0.125
- trailing_norm_gain: float32 [4096], P('kv'), may hold values from 0.1 to 1.9
- trailing_gate_weight: bfloat16 [4096, 11264], P('kv', ('dp', 'tp')), may hold values from -0.09375 to 0.09375
- trailing_up_weight: bfloat16 [4096, 11264], P('kv', ('dp', 'tp')), may hold values from -0.09375 to 0.09375
- trailing_down_weight: bfloat16 [11264, 4096], P(('dp', 'tp'), 'kv'), may hold values from -0.0546875 to 0.0546875
Outputs:
- result: bfloat16 [128, 4096], P(('grp', 'dp', 'tp'), 'kv'), parts along dimension 0
- new_state: float32 [128, 16, 64, 128], P(('grp', 'kv'), ('dp', 'tp')), parts along dimension 0
The draws below stay inside these ranges and needn't reach their ends.
There are 2 independent parts, one for each index of `grp`. The reference program is written for one: setup_inputs(seed, part) draws one part's arguments, and reference() takes and returns one part's arrays. A program takes and returns all parts, laid end to end along the dimension named above; an argument that names none is the same for every part. Nothing has to cross between parts.
All inputs are finite; a program needn't handle non-finite values.
Results may differ from the reference program's by a relative error of at most 0.0095.
Values may be sent and summed in bfloat16 or wider, within the bound.
A program may use at most 128 MiB of HBM per device.

```python
import jax
import jax.numpy as jnp
from jax import lax

D = 4096
FF = 11264
HEAD_COUNT = 16
KEY_CHANNELS = 64
VALUE_DIM = 128
BATCH_SIZE = 64


def shard_levels(stream_key, shape, split, low, largest):
    level, own = 1.0, jax.random.fold_in(stream_key, 6)
    for axis_at, parts in split:
        steps = jnp.exp(jax.random.uniform(jax.random.fold_in(own, axis_at), (parts,), jnp.float32, low / len(split), largest / len(split)))
        level = level * jnp.repeat(steps, shape[axis_at] // parts).reshape([-1 if axis == axis_at else 1 for axis in range(len(shape))])
    return level


def bell_draw(key, extent, spread, limit, cuts=(), held_as=jnp.bfloat16):
    factor_of = shard_levels(key, extent, cuts, -0.22, 0.18) if cuts else 1.0
    values = jax.random.normal(key, extent, jnp.float32) * spread * factor_of
    return jnp.minimum(jnp.maximum(values, -limit), limit).astype(held_as)


def setup_inputs(seed: int = 0, part: int = 0) -> dict:
    splits = jax.random.split(jax.random.key(seed), 20)
    own_keys = jax.random.split(jax.random.fold_in(splits[19], part), 20)
    return {
        "residual_input": bell_draw(own_keys[0], (BATCH_SIZE, D), 1.0, 6.0, ((0, 4), (1, 4))),
        "incoming_state": bell_draw(own_keys[1], (BATCH_SIZE, HEAD_COUNT, KEY_CHANNELS, VALUE_DIM), 0.5, 4.0, ((0, 4), (1, 4)), jnp.float32),
        "extra_log_decay": jnp.clip(-0.7 + 0.7 * jax.random.uniform(own_keys[2], (BATCH_SIZE, HEAD_COUNT * KEY_CHANNELS), jnp.float32) ** shard_levels(own_keys[2], (BATCH_SIZE, HEAD_COUNT * KEY_CHANNELS), ((0, 4), (1, 4)), -0.2, 0.2), -0.7, 0.0),
        "leading_norm_gain": jnp.clip(1.0 + 0.18 * jax.random.normal(splits[3], (D,), jnp.float32), 0.1, 1.9),
        "leading_gate_weight": bell_draw(splits[4], (D, FF), D ** -0.5, 0.09375, ((0, 4), (1, 4))),
        "leading_up_weight": bell_draw(splits[5], (D, FF), D ** -0.5, 0.09375, ((0, 4), (1, 4))),
        "leading_down_weight": bell_draw(splits[6], (FF, D), FF ** -0.5, 0.0546875, ((0, 4), (1, 4))),
        "attention_norm_gain": jnp.clip(1.0 + 0.18 * jax.random.normal(splits[7], (D,), jnp.float32), 0.1, 1.9),
        "query_projector": bell_draw(splits[8], (D, HEAD_COUNT * KEY_CHANNELS), D ** -0.5, 0.09375, ((0, 4), (1, 4))),
        "key_projector": bell_draw(splits[9], (D, HEAD_COUNT * KEY_CHANNELS), D ** -0.5, 0.09375, ((0, 4), (1, 4))),
        "value_projector": bell_draw(splits[10], (D, HEAD_COUNT * VALUE_DIM), D ** -0.5, 0.09375, ((0, 4), (1, 4))),
        "output_gate_weight": bell_draw(splits[11], (D, HEAD_COUNT * VALUE_DIM), D ** -0.5, 0.09375, ((0, 4), (1, 4))),
        "forget_weight": bell_draw(splits[12], (D, HEAD_COUNT * KEY_CHANNELS), (max(D // 64, 1)) ** -0.5, 0.75, ((0, 4), (1, 4))),
        "head_norm_gain": jnp.clip(1.0 + 0.18 * jax.random.normal(splits[13], (VALUE_DIM,), jnp.float32), 0.1, 1.9),
        "output_projector": bell_draw(splits[14], (HEAD_COUNT * VALUE_DIM, D), (HEAD_COUNT * VALUE_DIM) ** -0.5, 0.125, ((0, 4), (1, 4))),
        "trailing_norm_gain": jnp.clip(1.0 + 0.18 * jax.random.normal(splits[15], (D,), jnp.float32), 0.1, 1.9),
        "trailing_gate_weight": bell_draw(splits[16], (D, FF), D ** -0.5, 0.09375, ((0, 4), (1, 4))),
        "trailing_up_weight": bell_draw(splits[17], (D, FF), D ** -0.5, 0.09375, ((0, 4), (1, 4))),
        "trailing_down_weight": bell_draw(splits[18], (FF, D), FF ** -0.5, 0.0546875, ((0, 4), (1, 4))),
    }


epsilon = 1e-06

def row_scale(row_block):
    widened = row_block.astype(jnp.float32)
    return lax.rsqrt(lax.optimization_barrier(jnp.sum(widened * widened, axis=1, keepdims=True)) / D + epsilon)

def channel_mixer(row_block, norm_gain, gate_matrix, up_matrix, down_matrix):
    decay_factor = row_scale(row_block)
    scaled = (row_block.astype(jnp.float32) * norm_gain).astype(jnp.bfloat16)
    gate_sum = decay_factor * jnp.dot(scaled, gate_matrix, preferred_element_type=jnp.float32)
    up_sum = decay_factor * jnp.dot(scaled, up_matrix, preferred_element_type=jnp.float32)
    hidden = (jax.nn.silu(gate_sum) * up_sum).astype(jnp.bfloat16)
    return jnp.dot(hidden, down_matrix, preferred_element_type=jnp.float32)

def reference(residual_input, incoming_state, extra_log_decay, leading_norm_gain, leading_gate_weight, leading_up_weight, leading_down_weight, attention_norm_gain, query_projector, key_projector, value_projector, output_gate_weight, forget_weight, head_norm_gain, output_projector, trailing_norm_gain, trailing_gate_weight, trailing_up_weight, trailing_down_weight):
    after_first = (residual_input.astype(jnp.float32) + 0.5 * channel_mixer(residual_input, leading_norm_gain, leading_gate_weight, leading_up_weight, leading_down_weight)).astype(jnp.bfloat16)
    decay_factor = row_scale(after_first)
    scaled = (after_first.astype(jnp.float32) * attention_norm_gain).astype(jnp.bfloat16)

    def apply_projection(matrix):
        return decay_factor * jnp.dot(scaled, matrix, preferred_element_type=jnp.float32)
    queries = apply_projection(query_projector).reshape(BATCH_SIZE, HEAD_COUNT, KEY_CHANNELS) * KEY_CHANNELS ** (-0.5)
    key_rows = apply_projection(key_projector).reshape(BATCH_SIZE, HEAD_COUNT, KEY_CHANNELS)
    value_rows = apply_projection(value_projector).reshape(BATCH_SIZE, HEAD_COUNT, VALUE_DIM)
    gate_rows = apply_projection(output_gate_weight).reshape(BATCH_SIZE, HEAD_COUNT, VALUE_DIM)
    decay_logarithm = (jax.nn.log_sigmoid(apply_projection(forget_weight)) / 16.0 + extra_log_decay).reshape(BATCH_SIZE, HEAD_COUNT, KEY_CHANNELS)
    new_state = jnp.exp(decay_logarithm)[..., None] * incoming_state + key_rows[..., None] * value_rows[:, :, None, :]
    read_out = jnp.einsum('bhk,bhkv->bhv', queries, new_state, precision=lax.Precision.HIGHEST)
    normed = read_out * lax.rsqrt(lax.optimization_barrier(jnp.mean(read_out * read_out, axis=-1, keepdims=True)) + epsilon)
    head_rows = (normed * head_norm_gain * jax.nn.silu(gate_rows)).astype(jnp.bfloat16).reshape(BATCH_SIZE, HEAD_COUNT * VALUE_DIM)
    second = (after_first.astype(jnp.float32) + jnp.dot(head_rows, output_projector, preferred_element_type=jnp.float32)).astype(jnp.bfloat16)
    result = (second.astype(jnp.float32) + 0.5 * channel_mixer(second, trailing_norm_gain, trailing_gate_weight, trailing_up_weight, trailing_down_weight)).astype(jnp.bfloat16)
    return (result, new_state)
```

```python
import functools

import jax
import jax.numpy as jnp
from jax import lax
from jax.experimental import pallas as pl
from jax.experimental.pallas import tpu as pltpu
from jax.sharding import PartitionSpec as P

KEY_CHANNELS = 64
VALUE_DIM = 128
LANES = 128
epsilon = 1e-06
MESH = pl.DeviceIdType.MESH
F32 = jnp.float32
BF16 = jnp.bfloat16
CHUNKS = 4


def spans(width, count):
    if width % LANES:
        return [(0, width)]
    tile = 2 * LANES if width % (2 * LANES) == 0 else LANES
    tiles = width // tile
    count = min(count, tiles)
    cuts = [tile * ((tiles * i + count - 1) // count) for i in range(count + 1)]
    return list(zip(cuts[:-1], cuts[1:]))


def padded(width):
    return -(-width // LANES) * LANES


def silu(x):
    return x * jax.nn.sigmoid(x)


def kernel(dims, names, *refs):
    R, K, TP, D, B, d, F, W, V, heads = dims
    mr, mk = B // R, B // K
    ref = dict(zip(names, refs))
    dp_i, tp_i, k = lax.axis_index("dp"), lax.axis_index("tp"), lax.axis_index("kv")
    r = dp_i * TP + tp_i
    Wp = padded(W)
    kv_order = sorted(range(1, K), key=lambda o: abs(2 * o - K))
    counter = {"send": 0, "local": 0}
    pending = []

    def row_peer(o):
        t = lax.rem(r + o, R)
        return t, {"dp": t // TP, "tp": lax.rem(t, TP)}

    def kv_peer(o):
        t = lax.rem(k + o, K)
        return t, {"kv": t}

    def local(src, dst):
        i = counter["local"]
        counter["local"] += 1
        copy = pltpu.make_async_copy(src, dst, ref["local_sem"].at[i])
        copy.start()
        return copy

    def remote(src, dst, device):
        i = counter["send"]
        counter["send"] += 1
        copy = pltpu.make_async_remote_copy(
            src_ref=src,
            dst_ref=dst,
            send_sem=ref["send_sem"].at[i],
            recv_sem=ref["recv_sem"].at[i],
            device_id=device,
            device_id_type=MESH,
        )
        copy.start()
        pending.append(copy)
        return copy

    own_x = local(ref["x"], ref["x_all"].at[r])
    load_g1 = local(ref["g1"], ref["g1_v"])
    fspans = spans(F, CHUNKS)

    def load_mixer(p):
        first = []
        for a, b in fspans:
            cut = (slice(None), slice(None)) if b - a == F else (slice(None), pl.ds(a, b - a))
            first.append(
                (
                    local(ref[p + "g"].at[cut], ref[p + "g_v"].at[cut]),
                    local(ref[p + "u"].at[cut], ref[p + "u_v"].at[cut]),
                )
            )
        return first, local(ref[p + "d"], ref[p + "d_v"])

    lead = load_mixer("l")
    load_attn = [local(ref[n], ref[n + "_v"]) for n in ("g2", "wq", "wk", "wf", "wv", "wg")]
    load_state = [local(ref[n], ref[n + "_v"]) for n in ("st", "eld", "hng")]
    load_out = local(ref["wo"], ref["wo_v"])
    load_g3 = local(ref["g3"], ref["g3_v"])
    trail = load_mixer("t")

    barrier = pltpu.get_barrier_semaphore()
    for o in range(1, R):
        pl.semaphore_signal(barrier, inc=1, device_id=row_peer(o)[1], device_id_type=MESH)
    for o in kv_order:
        pl.semaphore_signal(barrier, inc=1, device_id=kv_peer(o)[1], device_id_type=MESH)
    pl.semaphore_wait(barrier, R - 1 + K - 1)

    def gather_rows(src, buf):
        copies = [remote(src, buf.at[r], row_peer(o)[1]) for o in range(1, R)]
        return copies

    def wait_all(copies):
        for copy in copies:
            copy.wait_recv()

    def normalised(buf, gain):
        wide = buf[...].reshape(B, d).astype(F32)
        squares = jnp.sum(wide * wide, axis=1, keepdims=True)
        ref["scaled"][...] = (wide * gain[...]).astype(BF16)
        return jnp.broadcast_to(squares, (B, LANES)).reshape(K, mk, LANES)

    def row_scale(total):
        return lax.rsqrt(total / D + epsilon)[:, :1]

    def mixer(p, buf, gain, loads):
        gu_loads, down_load = loads
        gu_send, gu_recv = ref[p + "gu_send"], ref[p + "gu_recv"]
        ss_send, ss_recv = ref[p + "ss_send"], ref[p + "ss_recv"]
        h_all = ref[p + "h_all"]
        ss_send[...] = normalised(buf, gain)
        ss_copies = []
        for o in kv_order:
            t, device = kv_peer(o)
            ss_copies.append(remote(ss_send.at[t], ss_recv.at[o - 1], device))
        gu_copies = []
        for (a, b), pair in zip(fspans, gu_loads):
            for i, part in enumerate("gu"):
                pair[i].wait()
                product = jnp.dot(
                    ref["scaled"][...], ref[p + part + "_v"][:, a:b], preferred_element_type=F32
                )
                gu_send[:, i, :, a:b] = product.astype(BF16).reshape(K, mk, b - a)
            group = []
            for o in kv_order:
                t, device = kv_peer(o)
                if b - a == F:
                    src, dst = gu_send.at[t], gu_recv.at[o - 1]
                else:
                    src = gu_send.at[t, :, :, pl.ds(a, b - a)]
                    dst = gu_recv.at[o - 1, :, :, pl.ds(a, b - a)]
                group.append(remote(src, dst, device))
            gu_copies.append(group)
        wait_all(ss_copies)
        total = ss_send[k]
        for o in kv_order:
            total = total + ss_recv[o - 1]
        scale = row_scale(total)
        h_copies = []
        for (a, b), group in zip(fspans, gu_copies):
            wait_all(group)
            gate = gu_send[k, 0, :, a:b].astype(F32)
            up = gu_send[k, 1, :, a:b].astype(F32)
            for o in kv_order:
                gate = gate + gu_recv[o - 1, 0, :, a:b].astype(F32)
                up = up + gu_recv[o - 1, 1, :, a:b].astype(F32)
            h_all[k, :, a:b] = (silu(scale * gate) * (scale * up)).astype(BF16)
            mine = h_all.at[k] if b - a == F else h_all.at[k, :, pl.ds(a, b - a)]
            h_copies.append([remote(mine, mine, kv_peer(o)[1]) for o in kv_order])
        down_load.wait()
        acc = None
        for (a, b), group in zip(fspans, h_copies):
            wait_all(group)
            part = jnp.dot(
                h_all[:, :, a:b].reshape(B, b - a),
                ref[p + "d_v"][a:b, :],
                preferred_element_type=F32,
            )
            acc = part if acc is None else acc + part
        return acc

    def scatter_rows(p, value):
        send, recv = ref[p + "_send"], ref[p + "_recv"]
        send[...] = value.astype(BF16).reshape(R, mr, d)
        copies = []
        for o in range(1, R):
            t, device = row_peer(o)
            copies.append(remote(send.at[t], recv.at[o - 1], device))
        wait_all(copies)
        total = send[r].astype(F32)
        for o in range(1, R):
            total = total + recv[o - 1].astype(F32)
        return total

    x_copies = gather_rows(ref["x"], ref["x_all"])
    own_x.wait()
    load_g1.wait()
    wait_all(x_copies)
    share = scatter_rows("p1", mixer("l", ref["x_all"], ref["g1_v"], lead))
    after = (ref["x_all"][r].astype(F32) + 0.5 * share).astype(BF16)
    ref["a_all"][r] = after
    a_copies = gather_rows(ref["a_all"].at[r], ref["a_all"])
    for copy in load_attn:
        copy.wait()
    wait_all(a_copies)

    squares = normalised(ref["a_all"], ref["g2_v"])
    f_send, f_recv = ref["f_send"], ref["f_recv"]
    q_send, q_recv = ref["q_send"], ref["q_recv"]
    v_send, v_recv = ref["v_send"], ref["v_recv"]

    def project(name):
        return jnp.dot(ref["scaled"][...], ref[name + "_v"][...], preferred_element_type=F32)

    f_send[:, :, Wp:] = squares
    f_send[:, :, :W] = project("wf").reshape(K, mk, W)
    f_copies, q_copies, v_copies = [], [], []
    for o in kv_order:
        t, device = kv_peer(o)
        f_copies.append(remote(f_send.at[t], f_recv.at[o - 1], device))
    q_send[:, 0, :, :W] = project("wq").astype(BF16).reshape(K, mk, W)
    q_send[:, 1, :, :W] = project("wk").astype(BF16).reshape(K, mk, W)
    for o in kv_order:
        t, device = kv_peer(o)
        q_copies.append(remote(q_send.at[t], q_recv.at[o - 1], device))
    v_send[:, 0] = project("wv").astype(BF16).reshape(K, mk, V)
    v_send[:, 1] = project("wg").astype(BF16).reshape(K, mk, V)
    for o in kv_order:
        t, device = kv_peer(o)
        v_copies.append(remote(v_send.at[t], v_recv.at[o - 1], device))
    for copy in load_state:
        copy.wait()
    wait_all(f_copies)
    forget = f_send[k]
    for o in kv_order:
        forget = forget + f_recv[o - 1]
    scale = row_scale(forget[:, Wp:])
    forget = scale * forget[:, :W]
    decay = jnp.exp(
        (jnp.minimum(forget, 0.0) - jnp.log1p(jnp.exp(-jnp.abs(forget)))) / 16.0 + ref["eld_v"][...]
    )
    columns = ref["columns"]
    columns[0] = decay.T
    wait_all(q_copies)
    pair = []
    for i in range(2):
        total = q_send[k, i, :, :W].astype(F32)
        for o in kv_order:
            total = total + q_recv[o - 1, i, :, :W].astype(F32)
        pair.append(scale * total)
    columns[1] = pair[1].T
    columns[2] = (pair[0] * KEY_CHANNELS ** (-0.5)).T
    wait_all(v_copies)
    pair = []
    for i in range(2):
        total = v_send[k, i].astype(F32)
        for o in kv_order:
            total = total + v_recv[o - 1, i].astype(F32)
        pair.append(scale * total)
    ref["vals"][...] = pair[0]
    gates = silu(pair[1])
    for b in range(mk):
        for h in range(heads):
            rows = slice(h * KEY_CHANNELS, (h + 1) * KEY_CHANNELS)
            lanes = slice(h * VALUE_DIM, (h + 1) * VALUE_DIM)
            new = (
                columns[0, rows, b : b + 1] * ref["st_v"][b, h]
                + columns[1, rows, b : b + 1] * ref["vals"][b : b + 1, lanes]
            )
            ref["ns_v"][b, h] = new
            ref["read"][b : b + 1, lanes] = jnp.sum(
                columns[2, rows, b : b + 1] * new, axis=0, keepdims=True
            )
    store_state = local(ref["ns_v"], ref["new_state"])
    hr_all = ref["hr_all"]
    for h in range(heads):
        lanes = slice(h * VALUE_DIM, (h + 1) * VALUE_DIM)
        out = ref["read"][:, lanes]
        out = out * lax.rsqrt(jnp.mean(out * out, axis=1, keepdims=True) + epsilon)
        hr_all[k, :, lanes] = (out * ref["hng_v"][...] * gates[:, lanes]).astype(BF16)
    hr_copies = [remote(hr_all.at[k], hr_all.at[k], kv_peer(o)[1]) for o in kv_order]
    load_out.wait()
    wait_all(hr_copies)
    mixed = scatter_rows(
        "p2",
        jnp.dot(hr_all[...].reshape(B, V), ref["wo_v"][...], preferred_element_type=F32),
    )
    second = (ref["a_all"][r].astype(F32) + mixed).astype(BF16)
    ref["s_all"][r] = second
    s_copies = gather_rows(ref["s_all"].at[r], ref["s_all"])
    load_g3.wait()
    wait_all(s_copies)

    share = scatter_rows("p3", mixer("t", ref["s_all"], ref["g3_v"], trail))
    ref["res_v"][...] = (ref["s_all"][r].astype(F32) + 0.5 * share).astype(BF16)
    store_result = local(ref["res_v"], ref["result"])
    for copy in pending:
        copy.wait_send()
    store_state.wait()
    store_result.wait()


ARGS = ("x", "st", "eld", "g1", "lg", "lu", "ld", "g2", "wq", "wk")
ARGS += ("wv", "wg", "wf", "hng", "wo", "g3", "tg", "tu", "td")


def per_device(sizes, *arrays):
    dp, tp, K = sizes
    R = dp * tp
    ref = dict(zip(ARGS, arrays))
    for n in ("g1", "g2", "g3", "hng"):
        ref[n] = ref[n].reshape(1, -1)
    mr, d = ref["x"].shape
    B, D = mr * R, d * K
    mk = B // K
    F = ref["lg"].shape[1]
    W, V = ref["wq"].shape[1], ref["wv"].shape[1]
    heads = W // KEY_CHANNELS
    Wp = padded(W)
    dims = (R, K, tp, D, B, d, F, W, V, heads)
    vm = {}
    for n in ARGS:
        if n != "x":
            vm[n + "_v"] = (ref[n].shape, ref[n].dtype)
    for n in ("x_all", "a_all", "s_all"):
        vm[n] = ((R, mr, d), BF16)
    vm["scaled"] = ((B, d), BF16)
    for p in ("l", "t"):
        vm[p + "gu_send"] = ((K, 2, mk, F), BF16)
        vm[p + "gu_recv"] = ((K - 1, 2, mk, F), BF16)
        vm[p + "ss_send"] = ((K, mk, LANES), F32)
        vm[p + "ss_recv"] = ((K - 1, mk, LANES), F32)
        vm[p + "h_all"] = ((K, mk, F), BF16)
    for p in ("p1", "p2", "p3"):
        vm[p + "_send"] = ((R, mr, d), BF16)
        vm[p + "_recv"] = ((R - 1, mr, d), BF16)
    vm["f_send"] = ((K, mk, Wp + LANES), F32)
    vm["f_recv"] = ((K - 1, mk, Wp + LANES), F32)
    vm["q_send"] = ((K, 2, mk, Wp), BF16)
    vm["q_recv"] = ((K - 1, 2, mk, Wp), BF16)
    vm["v_send"] = ((K, 2, mk, V), BF16)
    vm["v_recv"] = ((K - 1, 2, mk, V), BF16)
    vm["columns"] = ((3, W, mk), F32)
    vm["vals"] = ((mk, V), F32)
    vm["read"] = ((mk, V), F32)
    vm["ns_v"] = (ref["st"].shape, F32)
    vm["hr_all"] = ((K, mk, V), BF16)
    vm["res_v"] = ((mr, d), BF16)
    names = [*ARGS, "result", "new_state", *vm, "local_sem", "send_sem", "recv_sem"]
    sems = 3 * 2 * R + 2 * K * (1 + 2 * CHUNKS) + 4 * K
    return pl.pallas_call(
        functools.partial(kernel, dims, names),
        out_shape=(
            jax.ShapeDtypeStruct((mr, d), BF16),
            jax.ShapeDtypeStruct(ref["st"].shape, F32),
        ),
        in_specs=[pl.BlockSpec(memory_space=pl.ANY)] * len(ARGS),
        out_specs=[pl.BlockSpec(memory_space=pl.ANY)] * 2,
        scratch_shapes=[
            *[pltpu.VMEM(shape, dtype) for shape, dtype in vm.values()],
            pltpu.SemaphoreType.DMA((20 + 6 * CHUNKS,)),
            pltpu.SemaphoreType.DMA((sems,)),
            pltpu.SemaphoreType.DMA((sems,)),
        ],
        compiler_params=pltpu.CompilerParams(
            collective_id=0, has_side_effects=True, vmem_limit_bytes=63 * 1024 * 1024
        ),
    )(*[ref[n] for n in ARGS])


def solution(mesh):
    sizes = (mesh.shape["dp"], mesh.shape["tp"], mesh.shape["kv"])
    return jax.shard_map(
        functools.partial(per_device, sizes),
        mesh=mesh,
        in_specs=(
            P(("grp", "dp", "tp"), "kv"),
            P(("grp", "kv"), ("dp", "tp"), None, None),
            P(("grp", "kv"), ("dp", "tp")),
            P("kv"),
            P("kv", ("dp", "tp")),
            P("kv", ("dp", "tp")),
            P(("dp", "tp"), "kv"),
            P("kv"),
            P("kv", ("dp", "tp")),
            P("kv", ("dp", "tp")),
            P("kv", ("dp", "tp")),
            P("kv", ("dp", "tp")),
            P("kv", ("dp", "tp")),
            P(),
            P(("dp", "tp"), "kv"),
            P("kv"),
            P("kv", ("dp", "tp")),
            P("kv", ("dp", "tp")),
            P(("dp", "tp"), "kv"),
        ),
        out_specs=(P(("grp", "dp", "tp"), "kv"), P(("grp", "kv"), ("dp", "tp"), None, None)),
        check_vma=False,
    )
```
